512 devices in a mesh: sp: 32 (over z, core), tp: 16 (over y, x).
Axes of the slice: x: 4, y: 4, z: 16, core: 2. Of those that a mesh axis runs over, the one named last changes fastest.
Arguments:
- queries: bfloat16 [16384, 1024], P('sp', 'tp'), may hold values from -20 to 20
- key_vectors: bfloat16 [16384, 1024], P('sp', 'tp'), may hold values from -20 to 20
- value_vectors: bfloat16 [16384, 1024], P('sp', 'tp'), may hold values from -6 to 6
- log_gate_sums: float32 [16384, 16], P('sp', 'tp'), may hold values from -2343 to 0, as said below
- residual: bfloat16 [16384, 2048], P('sp', 'tp'), may hold values from -24 to 24
- out_weight: bfloat16 [1024, 2048], P(None, 'tp'), may hold values from -0.75 to 0.75
- norm_gain: bfloat16 [2048], replicated, may hold values from 0.099609375 to 1.8984375
- routes: int32 [16384, 2], P('sp'), may hold values from 0 to 127, all different within a row; in each aligned block of 512 rows (0 to 511, 512 to 1023, ...) at most 10 rows name the same one
- route_weight: float32 [16384, 2], P('sp'), may hold values from 0.5 to 1.5
- expert_gate: bfloat16 [128, 2048, 512], P('sp', None, 'tp'), may hold values from -0.125 to 0.125
- expert_up: bfloat16 [128, 2048, 512], P('sp', None, 'tp'), may hold values from -0.125 to 0.125
- expert_down: bfloat16 [128, 512, 2048], P('sp', None, 'tp'), may hold values from -0.25 to 0.25
- shared_gate: bfloat16 [2048, 512], P(None, 'tp'), may hold values from -0.125 to 0.125
- shared_up: bfloat16 [2048, 512], P(None, 'tp'), may hold values from -0.125 to 0.125
- shared_down: bfloat16 [512, 2048], P(None, 'tp'), may hold values from -0.25 to 0.25
Outputs:
- layer_out: bfloat16 [16384, 2048], P('sp', 'tp')
The draws below stay inside these ranges and needn't reach their ends.
Inputs may be any that keep to these rules, and one draw needn't show every extreme that they name: `log_gate_sums`: for each head the values do not rise along the positions. `routes`: each row names 2 different experts; among the rows of one index of sp no expert is named by more than 10 rows, a bound that some block reaches.
All inputs are finite; a program needn't handle non-finite values.
Results may differ from the reference program's by a relative error of at most 0.014.
Values may be sent and summed in bfloat16 or wider, within the bound.
No kernel may reach another device: no remote copies, remote signals or barrier semaphores. Data moves between devices by JAX's collectives and lax.ppermute only.
A program may use at most 64 MiB of HBM per device.

```python
import math
import jax
import jax.numpy as jnp
import numpy as np
from jax import lax

D = 2048
HEAD_TOTAL = 16
HDIM = 64
EF = 512
SH = 512
TOPK = 2
TOK_DEV = 512
TOKEN_TOTAL = 16384
EXPERTS = 128
CAP = 10
N_SP = 32


def attention_pair(key):
    base_key = jax.random.fold_in(key, 11)
    key_query, key_keys = jax.random.split(base_key, 2)
    width = HEAD_TOTAL * HDIM
    query_draw = 1.5 * jax.random.normal(key_query, (TOKEN_TOTAL, width), jnp.float32)
    key_draw = 1.5 * jax.random.normal(key_keys, (TOKEN_TOTAL, width), jnp.float32)
    return (jnp.clip(query_draw, -20.0, 20.0), jnp.clip(key_draw, -20.0, 20.0))


def draw_queries(key, part):
    return attention_pair(key)[0].astype(jnp.bfloat16)


def draw_key_vectors(key, part):
    return attention_pair(key)[1].astype(jnp.bfloat16)


def draw_log_gate_sums(key, part):
    key_a, key_b, key_c, random_key_fourth, random_key_fifth = jax.random.split(jax.random.fold_in(key, 23), 5)
    keep_share = 0.5
    slower_decay_heads = jax.random.bernoulli(key_a, keep_share, (HEAD_TOTAL,))
    rate = jnp.where(slower_decay_heads, 0.4 / TOKEN_TOTAL, 1.0 / 40.0)
    block_factor = 2.0 ** jax.random.uniform(key_b, (TOKEN_TOTAL // TOK_DEV, 1), jnp.float32, -1.0, 1.0)
    per_token = jnp.repeat(block_factor, TOK_DEV, axis=0)
    data_factor = jnp.exp(jax.random.uniform(key_c, (TOKEN_TOTAL, HEAD_TOTAL), jnp.float32, -1.0, 1.0))
    logarithm_decay_terms = -rate[None, :] * per_token * data_factor
    cluster_positions = jax.random.randint(random_key_fourth, (3,), 0, TOKEN_TOTAL)
    cluster_length = jnp.log(jax.random.uniform(random_key_fifth, (3, HEAD_TOTAL), jnp.float32, 0.5, 0.8))
    cluster_token_count = (jnp.arange(TOKEN_TOTAL, dtype=jnp.int32)[:, None] == cluster_positions[None, :]).astype(jnp.float32)
    token_clusters = jnp.sum(cluster_token_count[:, :, None] * cluster_length[None, :, :], axis=1)
    logarithm_decay_terms = logarithm_decay_terms + jnp.where(slower_decay_heads[None, :], token_clusters, 0.0)
    return jnp.cumsum(logarithm_decay_terms, axis=0)


def draw_residual(key, part):
    key_a = jax.random.fold_in(jax.random.fold_in(key, 31), 0)
    key_c = jax.random.fold_in(jax.random.fold_in(key, 31), 2)
    column = jnp.arange(D, dtype=jnp.float32) / D
    base_draw = jax.random.normal(key_a, (TOKEN_TOTAL, D), jnp.float32)
    col_scale = 0.4 * 5.0 ** column * jax.random.uniform(key_c, (D,), jnp.float32, 0.7, 1.3)
    values = col_scale[None, :] * base_draw
    return jnp.clip(values, -24.0, 24.0).astype(jnp.bfloat16)


def block_scale(key, extent, shards, least, top_value):
    loudness = 1.0
    for axis_at, parts in shards:
        draws = jax.random.uniform(jax.random.fold_in(jax.random.fold_in(key, 6), axis_at), (parts,), jnp.float32, least / len(shards), top_value / len(shards))
        loudness = loudness * jnp.repeat(jnp.exp(draws), extent[axis_at] // parts).reshape((-1,) + (1,) * (len(extent) - 1 - axis_at))
    return loudness


def deal_out(stream_key, own, number, rows, amount, top, bound, lean):
    ranking = jax.random.permutation(stream_key, amount)
    packed, common = portions_of(amount, rows * top, bound, lean, True), portions_of(amount, rows * top, bound, lean, False)
    places = jnp.arange(amount)

    def named(lengths, rotation):
        used = int((lengths > 0).sum())
        fixed = max(1, used // 4)
        shifted = fixed + (places - fixed + rotation * (used - fixed)) % max(1, amount - fixed)
        return jnp.zeros((amount,), jnp.int32).at[ranking[jnp.where(places < fixed, places, shifted)]].set(jnp.asarray(lengths, jnp.int32))

    lengths = jnp.where(number % 4 == 0, named(packed, number // 4), named(common, number - number // 4 - 1))
    mixed = jax.random.permutation(jax.random.fold_in(own, 3), amount)
    donor, sink = mixed[0:amount // 2 * 2:2], mixed[1:amount // 2 * 2:2]
    slack = jnp.minimum(lengths[donor] - 1, bound - lengths[sink]) // 2
    slack = jnp.where((donor == ranking[0]) | (sink == ranking[0]) | (lengths[sink] == 0), 0, jnp.maximum(slack, 0))
    shifted = jax.random.randint(jax.random.fold_in(own, 4), (amount // 2,), 0, 1 << 20) % (slack + 1)
    lengths = lengths.at[donor].add(-shifted).at[sink].add(shifted)
    members = jnp.searchsorted(jnp.cumsum(lengths), jnp.arange(rows * top), side="right").astype(jnp.int32)
    grid = members.reshape(top, rows).T
    grid = grid[jax.random.permutation(jax.random.fold_in(own, 1), rows)]
    rotation = jax.random.randint(jax.random.fold_in(own, 2), (rows, 1), 0, top)
    return jnp.take_along_axis(grid, (jnp.arange(top)[None, :] + rotation) % top, axis=1)


def portions_of(count, total, limit, lean, full):
    loads = [(1 << 20) // math.isqrt(grade ** lean) + 1 for grade in range(1, count + 1)]
    largest = limit if full else min(limit, max(-(-total // count), total * loads[0] // sum(loads)))
    least = 1 if total - largest >= count - 1 else 0
    counts, rest = [largest] + [least] * (count - 1), total - largest - least * (count - 1)
    while rest > 0:
        free = [i for i in range(1, count) if counts[i] < largest] or [i for i in range(1, count) if counts[i] < limit]
        mass, budget = sum([loads[i] for i in free]), rest
        for i in free:
            extra = min(limit - counts[i], max(1, budget * loads[i] // mass), rest)
            counts[i] = counts[i] + extra
            rest = rest - extra
    return np.array(counts)


def normal_values(rng, extent, deviation, bound, pieces=(), kind=jnp.bfloat16):
    loudness = block_scale(rng, extent, pieces, -0.22, 0.18) if pieces else 1.0
    entries = jax.random.normal(rng, extent, jnp.float32) * deviation * loudness
    return jnp.minimum(jnp.maximum(entries, -bound), bound).astype(kind)


def setup_inputs(seed: int = 0) -> dict:
    keys = jax.random.split(jax.random.key(seed), 16)
    queries = draw_queries(jax.random.fold_in(keys[15], 71), 0)
    key_vectors = draw_key_vectors(jax.random.fold_in(keys[15], 71), 0)
    value_vectors = normal_values(keys[2], (TOKEN_TOTAL, HEAD_TOTAL * HDIM), 1.0, 6.0, ((0, 32), (1, 16)))
    log_gate_sums = draw_log_gate_sums(jax.random.fold_in(keys[15], 71), 0)
    residual = draw_residual(jax.random.fold_in(keys[15], 71), 0)
    out_weight = normal_values(keys[5], (HEAD_TOTAL * HDIM, D), (HEAD_TOTAL * HDIM // 16) ** -0.5, 0.75, ((1, 16),))
    norm_gain = jnp.clip(1.0 + 0.18 * jax.random.normal(keys[6], (D,), jnp.float32), 0.099609375, 1.8984375).astype(jnp.bfloat16)
    routes_keys = jax.random.split(jax.random.fold_in(keys[7], 1), TOKEN_TOTAL // TOK_DEV)
    routes_turns = jax.random.permutation(jax.random.fold_in(keys[7], 3), TOKEN_TOTAL // TOK_DEV)
    routes = jax.vmap(lambda own, number: deal_out(jax.random.fold_in(keys[7], 2), own, number, TOK_DEV, EXPERTS, TOPK, CAP, 1))(routes_keys, routes_turns).reshape((TOKEN_TOTAL, TOPK))
    route_weight = jnp.clip(0.5 + 1.0 * jax.random.uniform(keys[8], (TOKEN_TOTAL, TOPK), jnp.float32) ** block_scale(keys[8], (TOKEN_TOTAL, TOPK), ((0, 32),), -0.2, 0.2), 0.5, 1.5)
    expert_gate = normal_values(keys[9], (EXPERTS, D, EF), D ** -0.5, 0.125, ((0, 32), (2, 16)))
    expert_up = normal_values(keys[10], (EXPERTS, D, EF), D ** -0.5, 0.125, ((0, 32), (2, 16)))
    expert_down = normal_values(keys[11], (EXPERTS, EF, D), EF ** -0.5, 0.25, ((0, 32), (2, 16)))
    shared_gate = normal_values(keys[12], (D, SH), D ** -0.5, 0.125, ((1, 16),))
    shared_up = normal_values(keys[13], (D, SH), D ** -0.5, 0.125, ((1, 16),))
    shared_down = normal_values(keys[14], (SH, D), SH ** -0.5, 0.25, ((1, 16),))
    return dict(queries=queries, key_vectors=key_vectors, value_vectors=value_vectors, log_gate_sums=log_gate_sums, residual=residual, out_weight=out_weight, norm_gain=norm_gain, routes=routes, route_weight=route_weight, expert_gate=expert_gate, expert_up=expert_up, expert_down=expert_down, shared_gate=shared_gate, shared_up=shared_up, shared_down=shared_down)


EPSILON = 1e-06

def silu_gate(gate_part, up_part):
    return jax.nn.silu(gate_part) * up_part

def one_head(inputs):
    query_head, key_head, value_head, gate_head = inputs
    block_size = math.gcd(TOKEN_TOTAL, 512)
    key_pos = jnp.arange(TOKEN_TOTAL, dtype=jnp.int32)
    score_scale = HDIM ** (-0.5)

    def one_block(block_number):
        first_row = (block_number * block_size).astype(jnp.int32)
        query_block = lax.dynamic_slice_in_dim(query_head, first_row, block_size, 0)
        gate_block = lax.dynamic_slice_in_dim(gate_head, first_row, block_size, 0)
        scores = jnp.dot(query_block, key_head.T, preferred_element_type=jnp.float32) * score_scale
        scores = scores + gate_block[:, None] - gate_head[None, :]
        query_pos = first_row + jnp.arange(block_size, dtype=jnp.int32)
        allowed = key_pos[None, :] <= query_pos[:, None]
        highest = lax.optimization_barrier(jnp.max(jnp.where(allowed, scores, -jnp.inf), axis=1, keepdims=True))
        weight = jnp.where(allowed, jnp.exp(scores - highest), 0.0)
        weight_total = lax.optimization_barrier(jnp.sum(weight, axis=1, keepdims=True))
        mixed_rows = jnp.dot(weight.astype(jnp.bfloat16), value_head, preferred_element_type=jnp.float32)
        return (mixed_rows / weight_total).astype(jnp.bfloat16)
    blocks_out = lax.map(one_block, jnp.arange(TOKEN_TOTAL // block_size, dtype=jnp.int32))
    return blocks_out.reshape(TOKEN_TOTAL, HDIM)

def block_targets(block_routes):
    flat_routes = block_routes.reshape(-1)
    onehot = (flat_routes[:, None] == jnp.arange(EXPERTS, dtype=jnp.int32)[None, :]).astype(jnp.int32)
    before = jnp.cumsum(onehot, axis=0) - onehot
    return flat_routes * CAP + lax.optimization_barrier(jnp.sum(before * onehot, axis=1))

def reference(queries, key_vectors, value_vectors, log_gate_sums, residual, out_weight, norm_gain, routes, route_weight, expert_gate, expert_up, expert_down, shared_gate, shared_up, shared_down):

    def by_head(matrix):
        return matrix.reshape(TOKEN_TOTAL, HEAD_TOTAL, HDIM).transpose(1, 0, 2)
    attended = lax.map(one_head, (by_head(queries), by_head(key_vectors), by_head(value_vectors), log_gate_sums.T))
    attended = attended.transpose(1, 0, 2).reshape(TOKEN_TOTAL, HEAD_TOTAL * HDIM)
    projected = jnp.dot(attended, out_weight, preferred_element_type=jnp.float32)
    mid = (residual.astype(jnp.float32) + projected).astype(jnp.bfloat16)
    mid_wide = mid.astype(jnp.float32)
    inverse = lax.rsqrt(lax.optimization_barrier(jnp.mean(mid_wide * mid_wide, axis=1, keepdims=True)) + EPSILON)
    normed = (mid_wide * inverse * norm_gain.astype(jnp.float32)).astype(jnp.bfloat16)
    shared_mid = silu_gate(jnp.dot(normed, shared_gate, preferred_element_type=jnp.float32), jnp.dot(normed, shared_up, preferred_element_type=jnp.float32)).astype(jnp.bfloat16)
    shared_out = jnp.dot(shared_mid, shared_down, preferred_element_type=jnp.float32)
    targets = jax.vmap(block_targets)(routes.reshape(N_SP, TOK_DEV, TOPK))
    local_rows = jnp.arange(TOK_DEV * TOPK, dtype=jnp.int32) // TOPK

    def block_owners(target_row, block_number):
        table = jnp.full((EXPERTS * CAP,), TOKEN_TOTAL, jnp.int32)
        return table.at[target_row].set(block_number * TOK_DEV + local_rows)
    owners = jax.vmap(block_owners)(targets, jnp.arange(N_SP, dtype=jnp.int32))
    owners = owners.reshape(N_SP, EXPERTS, CAP).transpose(1, 0, 2).reshape(EXPERTS, N_SP * CAP)
    padded = jnp.concatenate([normed, jnp.zeros((1, D), jnp.bfloat16)], axis=0)

    def one_expert(inputs):
        gate_weight, up_weight, down_weight, owner_rows = inputs
        row_values = padded[owner_rows]
        hidden = silu_gate(jnp.dot(row_values, gate_weight, preferred_element_type=jnp.float32), jnp.dot(row_values, up_weight, preferred_element_type=jnp.float32)).astype(jnp.bfloat16)
        return jnp.dot(hidden, down_weight, preferred_element_type=jnp.float32).astype(jnp.bfloat16)
    produced = lax.map(one_expert, (expert_gate, expert_up, expert_down, owners))
    expert_ids = targets // CAP
    slot_rank = targets % CAP
    block_ids = jnp.arange(N_SP, dtype=jnp.int32)[:, None]
    flat_index = (expert_ids * (N_SP * CAP) + block_ids * CAP + slot_rank).reshape(-1)
    picked = produced.reshape(EXPERTS * N_SP * CAP, D)[flat_index].astype(jnp.float32).reshape(TOKEN_TOTAL, TOPK, D)
    routed = lax.optimization_barrier(jnp.sum(picked * route_weight[:, :, None], axis=1))
    return (mid_wide + shared_out + routed).astype(jnp.bfloat16)
```

```python
import jax
import jax.numpy as jnp
from jax import lax
from jax.experimental import pallas as pl
from jax.experimental.pallas import tpu as pltpu
from jax.sharding import Mesh, PartitionSpec as P

HDIM = 64
EPSILON = 1e-06
CAPACITY = 10
BF = jnp.bfloat16
F32 = jnp.float32
NN = (((1,), (0,)), ((), ()))
NT = (((1,), (1,)), ((), ()))
TN = (((0,), (0,)), ((), ()))


def dot(a, b, dims=NN):
    return lax.dot_general(a, b, dims, preferred_element_type=F32)


def call(kernel, outs, *args, smem=0, scratch=(), flops=2**28, nbytes=2**22):
    specs = [pl.BlockSpec(memory_space=pltpu.SMEM)] * smem
    specs += [pl.BlockSpec(memory_space=pltpu.VMEM)] * (len(args) - smem)
    return pl.pallas_call(
        kernel,
        out_shape=outs,
        in_specs=specs,
        out_specs=jax.tree.map(lambda _: pl.BlockSpec(memory_space=pltpu.VMEM), outs),
        scratch_shapes=scratch,
        cost_estimate=pl.CostEstimate(flops=flops, bytes_accessed=nbytes, transcendentals=0),
    )(*args)


def shape(dims, dtype=BF):
    return jax.ShapeDtypeStruct(dims, dtype)


def fold(block, query, top, acc, mask=None):
    scores = dot(block[0:72], query, TN)
    if mask is not None:
        scores = jnp.where(mask, scores, -1e30)
    new_top = jnp.maximum(top, jnp.max(scores, axis=0, keepdims=True))
    weight = jnp.exp(scores - new_top).astype(BF)
    acc = acc * jnp.exp(top - new_top) + dot(block[64:136], weight)
    return new_top, acc


def own_kernel(block_ref, query_ref, top_ref, acc_ref):
    tokens = query_ref.shape[1]
    half = tokens // 2
    for part in range(2):
        cols = slice(part * half, (part + 1) * half)
        keys = (part + 1) * half
        key_at = lax.broadcasted_iota(jnp.int32, (keys, half), 0)
        query_at = lax.broadcasted_iota(jnp.int32, (keys, half), 1) + part * half
        top, acc = fold(
            block_ref[:, 0:keys],
            query_ref[:, cols],
            jnp.full((1, half), -1e30, F32),
            jnp.zeros((72, half), F32),
            key_at <= query_at,
        )
        top_ref[:, cols] = top
        acc_ref[:, cols] = acc


def past_kernel(last, count_ref, blocks_ref, query_ref, top_in, acc_in, *out_refs):
    tokens = query_ref.shape[1]
    half = tokens // 2
    if last:
        out_ref, top_ref, acc_ref = out_refs
    else:
        top_ref, acc_ref = out_refs
    top_ref[...] = top_in[...]
    acc_ref[...] = acc_in[...]

    def step(at, carry):
        block = blocks_ref[at]
        for part in range(2):
            cols = slice(part * half, (part + 1) * half)
            top, acc = fold(block, query_ref[:, cols], top_ref[:, cols], acc_ref[:, cols])
            top_ref[:, cols] = top
            acc_ref[:, cols] = acc
        return carry

    lax.fori_loop(0, count_ref[0], step, 0)
    if last:
        out_ref[...] = (acc_ref[8:72] / acc_ref[3:4]).astype(BF)


def slots_kernel(routes_ref, targets_ref):
    experts, tokens = 128, routes_ref.shape[1]
    expert_at = lax.broadcasted_iota(jnp.int32, (experts, tokens), 0)
    earlier = (
        lax.broadcasted_iota(jnp.int32, (tokens, tokens), 0)
        < lax.broadcasted_iota(jnp.int32, (tokens, tokens), 1)
    ).astype(F32).astype(BF)
    used = jnp.zeros((experts, 1), F32)
    for k in range(2):
        named = routes_ref[k : k + 1] == expert_at
        hot = named.astype(F32)
        before = dot(hot.astype(BF), earlier) + used
        rank = jnp.sum(jnp.where(named, before, 0.0), axis=0, keepdims=True)
        targets_ref[k : k + 1] = routes_ref[k : k + 1] * CAPACITY + rank.astype(jnp.int32)
        used = used + jnp.sum(hot, axis=1, keepdims=True)


def mid_kernel(heads_ref, weight_ref, residual_ref, mid_ref, squares_ref):
    projected = dot(weight_ref[...], heads_ref[...])
    mid = (residual_ref[...].astype(F32) + projected).astype(BF)
    mid_ref[...] = mid
    wide = mid.astype(F32)
    squares_ref[...] = jnp.broadcast_to(
        jnp.sum(wide * wide, axis=0, keepdims=True)[None], squares_ref.shape
    )


def hot_slots(targets_ref, k, first, rows):
    tokens = targets_ref.shape[1]
    slot_at = lax.broadcasted_iota(jnp.int32, (rows, tokens), 0) + first
    return targets_ref[k : k + 1] == slot_at


def normed_kernel(width, mid_ref, squares_ref, gain_ref, targets_ref, rows_ref, normed_ref):
    total = jnp.sum(squares_ref[...], axis=0)
    inverse = lax.rsqrt(total / width + EPSILON)
    normed = (mid_ref[...].astype(F32) * inverse * gain_ref[...]).astype(BF)
    normed_ref[...] = normed.astype(F32).T.astype(BF)
    chunk = rows_ref.shape[0] // 4
    for part in range(4):
        hot = hot_slots(targets_ref, 0, part * chunk, chunk) | hot_slots(
            targets_ref, 1, part * chunk, chunk
        )
        rows_ref[part * chunk : (part + 1) * chunk] = dot(
            hot.astype(F32).astype(BF), normed, NT
        ).astype(BF)


def sorting():
    to = lax.broadcasted_iota(jnp.int32, (320, 320), 0)
    frm = lax.broadcasted_iota(jnp.int32, (320, 320), 1)
    el = (to >= 80).astype(jnp.int32) + (to >= 160).astype(jnp.int32) + (to >= 240).astype(jnp.int32)
    within = to - el * 80
    src = jnp.zeros_like(to)
    for s in range(1, 8):
        src = src + (within >= s * 10).astype(jnp.int32)
    return (frm == src * 40 + el * 10 + within - src * 10).astype(F32).astype(BF)


def spread_kernel(arrived_ref, normed_ref, out_ref):
    order = sorting()
    for group in range(4):
        rows = dot(order, arrived_ref[group * 320 : (group + 1) * 320]).astype(BF)
        for el in range(4):
            piece = rows[el * 80 : (el + 1) * 80]
            for y in range(4):
                out_ref[y * 4 + el, group * 80 : (group + 1) * 80] = piece
    for x in range(4):
        piece = normed_ref[x * 128 : (x + 1) * 128]
        for y in range(4):
            out_ref[y * 4 + x, 320:448] = piece


def hidden_kernel(rows_ref, weight_ref, out_ref):
    expert = jnp.zeros((320, 256), F32)
    shared = jnp.zeros((128, 256), F32)

    def weights(first, cols):
        return jnp.concatenate(
            [weight_ref[x, g : g + 32, cols] for g in (first, first + 32) for x in range(4)], axis=0
        )

    for t in range(0, 16, 2):
        cols = slice(t * 128, (t + 2) * 128)
        rows = jnp.concatenate([rows_ref[t], rows_ref[t + 1]], axis=1)
        expert = expert + dot(rows[0:320], weights(0, cols), NT)
        shared = shared + dot(rows[320:448], weights(64, cols), NT)
    for first, count, both in ((0, 320, expert), (320, 128, shared)):
        gate, up = both[:, 0:128], both[:, 128:256]
        hidden = (gate / (1.0 + jnp.exp(-gate)) * up).astype(BF)
        for t in range(16):
            out_ref[t, first : first + count] = hidden


def down_kernel(hidden_ref, weight_ref, shared_ref, out_ref, shared_out_ref):
    order = sorting()
    produced = []
    for x in range(4):
        rows = jnp.zeros((320, 128), F32)
        shared = jnp.zeros((128, 128), F32)
        for y in range(0, 4, 2):
            cols = slice(y * 128, (y + 2) * 128)
            both = jnp.concatenate([hidden_ref[y * 4 + x], hidden_ref[y * 4 + 4 + x]], axis=1)
            rows = rows + dot(both[0:320], weight_ref[x, cols])
            shared = shared + dot(both[320:448], shared_ref[cols])
        produced.append(rows.astype(BF))
        shared_out_ref[x * 128 : (x + 1) * 128] = shared
    for group in range(4):
        rows = jnp.concatenate([p[group * 80 : (group + 1) * 80] for p in produced], axis=0)
        out_ref[group * 320 : (group + 1) * 320] = dot(order, rows, TN).astype(BF)


def last_kernel(returned_ref, targets_ref, weight_ref, mid_ref, shared_ref, out_ref):
    tokens = targets_ref.shape[1]
    total = mid_ref[...].astype(F32)
    slots = returned_ref.shape[0]
    chunk = slots // 5
    picked = [jnp.zeros(mid_ref.shape, F32) for _ in range(2)]
    for part in range(5):
        rows = returned_ref[part * chunk : (part + 1) * chunk]
        for k in range(2):
            hot = hot_slots(targets_ref, k, part * chunk, chunk).astype(F32).astype(BF)
            picked[k] = picked[k] + dot(rows, hot, TN)
    for k in range(2):
        total = total + picked[k] * weight_ref[k : k + 1]
    out_ref[...] = (total.T + shared_ref[...]).astype(BF)


def pieces(value):
    parts = []
    for _ in range(3):
        part = lax.reduce_precision(value, 8, 7)
        parts.append(part)
        value = value - part
    return jnp.concatenate(parts, axis=0).astype(BF)


def exchange(array, axis):
    return lax.all_to_all(array, axis, split_axis=0, concat_axis=0, tiled=True)


def shards(
    queries,
    key_vectors,
    value_vectors,
    log_gate_sums,
    residual,
    out_weight,
    norm_gain,
    routes,
    route_weight,
    expert_gate,
    expert_up,
    expert_down,
    shared_gate,
    shared_up,
    shared_down,
):
    tokens = queries.shape[0]
    width = norm_gain.shape[0]
    z, c = lax.axis_index("z"), lax.axis_index("c")
    tp = ("y", "x")
    gates = log_gate_sums.T
    ones = jnp.ones((3, tokens), BF)
    zeros = jnp.zeros((2, tokens), BF)
    block = jnp.concatenate(
        [key_vectors.T, pieces(-gates), ones, zeros, value_vectors.T], axis=0
    )
    gathered = lax.all_gather(block, "z", axis=0, tiled=False)
    query = jnp.concatenate([queries.T * BF(HDIM**-0.5), ones, pieces(gates), zeros], axis=0)
    state = (shape((1, tokens), F32), shape((72, tokens), F32))
    top, acc = call(own_kernel, state, block, query)

    local = jnp.stack([expert_gate, expert_up], axis=1).transpose(0, 1, 3, 2).reshape(4, 64, width)
    both = jnp.concatenate([shared_gate.T, shared_up.T], axis=0)
    local = jnp.concatenate([local, jnp.broadcast_to(both[None], (4, 64, width))], axis=1)
    up_weight = exchange(local, "x")
    targets = call(slots_kernel, shape((2, tokens), jnp.int32), routes.T)
    at = (lax.axis_index("y") * 4 + lax.axis_index("x")) * 128
    gain = lax.dynamic_slice_in_dim(norm_gain, at, 128, 0).astype(F32)[:, None]

    partner = lax.ppermute(gathered, "c", [(0, 1), (1, 0)])
    top, acc = call(
        lambda *refs: past_kernel(False, *refs), state, z.reshape(1), gathered, query, top, acc, smem=1
    )
    attended, _, _ = call(
        lambda *refs: past_kernel(True, *refs),
        (shape((HDIM, tokens)), *state),
        (z + c).reshape(1),
        partner,
        query,
        top,
        acc,
        smem=1,
    )
    heads = exchange(jnp.broadcast_to(attended[None], (16, HDIM, tokens)), tp)
    mid, squares = call(
        mid_kernel,
        (shape((128, tokens)), shape((16, 1, tokens), F32)),
        heads.reshape(16 * HDIM, tokens),
        out_weight.T,
        residual.T,
    )
    squares = exchange(squares, tp)
    rows, normed = call(
        lambda *refs: normed_kernel(width, *refs),
        (shape((1280, 128)), shape((tokens, 128))),
        mid,
        squares,
        gain,
        targets,
    )
    arrived = exchange(rows.reshape(32, 40, 128), ("z", "c")).reshape(1280, 128)
    spread = exchange(call(spread_kernel, shape((16, 448, 128)), arrived, normed), tp)
    hidden = exchange(call(hidden_kernel, shape((16, 448, 128)), spread, up_weight), tp)
    produced, shared = call(
        down_kernel,
        (shape((1280, 128)), shape((tokens, 128), F32)),
        hidden,
        expert_down,
        shared_down,
    )
    returned = exchange(produced.reshape(32, 40, 128), ("z", "c")).reshape(1280, 128)
    return call(
        last_kernel, shape((tokens, 128)), returned, targets, route_weight.T, mid, shared
    )


def solution(mesh):
    grid = Mesh(mesh.devices.reshape(16, 2, 4, 4), ("z", "c", "y", "x"))
    sp, tp = ("z", "c"), ("y", "x")
    placed = (
        P(sp, tp),
        P(sp, tp),
        P(sp, tp),
        P(sp, tp),
        P(sp, tp),
        P(None, tp),
        P(),
        P(sp, None),
        P(sp, None),
        P(sp, None, tp),
        P(sp, None, tp),
        P(sp, None, tp),
        P(None, tp),
        P(None, tp),
        P(None, tp),
    )
    return jax.shard_map(
        shards, mesh=grid, in_specs=placed, out_specs=P(sp, tp), check_vma=False
    )
```

```python
import functools

import jax
import jax.numpy as jnp
from jax import lax
from jax.experimental import pallas as pl
from jax.experimental.pallas import tpu as pltpu
from jax.sharding import Mesh, PartitionSpec as P

HDIM = 64
EPSILON = 1e-06
CAPACITY = 10
BF = jnp.bfloat16
F32 = jnp.float32
NN = (((1,), (0,)), ((), ()))
NT = (((1,), (1,)), ((), ()))
TN = (((0,), (0,)), ((), ()))


def dot(a, b, dims=NN):
    return lax.dot_general(a, b, dims, preferred_element_type=F32)


def call(kernel, outs, *args, smem=0, scratch=(), flops=2**28, nbytes=2**22):
    specs = [pl.BlockSpec(memory_space=pltpu.SMEM)] * smem
    specs += [pl.BlockSpec(memory_space=pltpu.VMEM)] * (len(args) - smem)
    return pl.pallas_call(
        kernel,
        out_shape=outs,
        in_specs=specs,
        out_specs=jax.tree.map(lambda _: pl.BlockSpec(memory_space=pltpu.VMEM), outs),
        scratch_shapes=scratch,
        cost_estimate=pl.CostEstimate(flops=flops, bytes_accessed=nbytes, transcendentals=0),
    )(*args)


def shape(dims, dtype=BF):
    return jax.ShapeDtypeStruct(dims, dtype)


def fold(block, query_ref, top_ref, acc_ref, parts):
    half = query_ref.shape[1] // 4
    columns = [slice(part * half, (part + 1) * half) for part in parts]
    keys = block[0:72].astype(F32).T.astype(BF)
    scores = [dot(keys, query_ref[:, cols]) for cols in columns]
    old = [top_ref[:, cols] for cols in columns]
    new = [jnp.maximum(o, jnp.max(s, axis=0, keepdims=True)) for o, s in zip(old, scores)]
    weights = [jnp.exp(s - n).astype(BF) for s, n in zip(scores, new)]
    values = [
        acc_ref[:, cols] * jnp.exp(o - n) + dot(block[64:136], w)
        for cols, o, n, w in zip(columns, old, new, weights)
    ]
    for cols, n, v in zip(columns, new, values):
        top_ref[:, cols] = n
        acc_ref[:, cols] = v


def own_kernel(core_ref, block_ref, query_ref, top_ref, acc_ref):
    tokens = block_ref.shape[1]
    half = tokens // 2
    for part in range(2):
        cols = slice(part * half, (part + 1) * half)
        keys = (part + 1) * half
        key_at = lax.broadcasted_iota(jnp.int32, (keys, half), 0)
        query_at = lax.broadcasted_iota(jnp.int32, (keys, half), 1) + part * half
        scores = dot(block_ref[0:72, 0:keys], query_ref[:, cols], TN)
        scores = jnp.where(key_at <= query_at, scores, -1e30)
        top = jnp.max(scores, axis=0, keepdims=True)
        top_ref[:, cols] = top
        acc_ref[:, cols] = dot(block_ref[64:136, 0:keys], jnp.exp(scores - top).astype(BF))
    top_ref[:, tokens:] = jnp.full((1, tokens), -1e30, F32)
    acc_ref[:, tokens:] = jnp.zeros((72, tokens), F32)

    @pl.when(core_ref[0] == 0)
    def _():
        fold(block_ref[...], query_ref, top_ref, acc_ref, (2, 3))


def past_kernel(k, chips, count, chip_ref, *refs):
    blocks, query_ref = refs[0:count], refs[count]
    top_in, acc_in, top_ref, acc_ref = refs[1 + count : 5 + count]
    top_ref[...] = top_in[...]
    acc_ref[...] = acc_in[...]
    chip = chip_ref[0]
    for useful, block_ref in zip((chip >= k, chip + k >= chips), blocks):

        @pl.when(useful)
        def _():
            fold(block_ref[...], query_ref, top_ref, acc_ref, range(4))

    if count == 1:
        sent_ref = refs[5 + count]
        tokens = sent_ref.shape[1]
        sent_ref[0:72] = acc_ref[:, tokens:]
        sent_ref[72:80] = jnp.broadcast_to(top_ref[:, tokens:], (8, tokens))


def merge_kernel(top_ref, acc_ref, other_ref, out_ref):
    tokens = out_ref.shape[2]
    top, other = top_ref[:, 0:tokens], other_ref[72:73]
    both = jnp.maximum(top, other)
    acc = acc_ref[:, 0:tokens] * jnp.exp(top - both) + other_ref[0:72] * jnp.exp(other - both)
    attended = (acc[8:72] / acc[3:4]).astype(BF)
    for t in range(16):
        out_ref[t] = attended


def slots_kernel(routes_ref, targets_ref):
    experts, tokens = 128, routes_ref.shape[1]
    expert_at = lax.broadcasted_iota(jnp.int32, (experts, tokens), 0)
    earlier = (
        lax.broadcasted_iota(jnp.int32, (tokens, tokens), 0)
        < lax.broadcasted_iota(jnp.int32, (tokens, tokens), 1)
    ).astype(F32).astype(BF)
    used = jnp.zeros((experts, 1), F32)
    for k in range(2):
        named = routes_ref[k : k + 1] == expert_at
        hot = named.astype(F32)
        before = dot(hot.astype(BF), earlier) + used
        rank = jnp.sum(jnp.where(named, before, 0.0), axis=0, keepdims=True)
        targets_ref[k : k + 1] = routes_ref[k : k + 1] * CAPACITY + rank.astype(jnp.int32)
        used = used + jnp.sum(hot, axis=1, keepdims=True)


def mid_kernel(heads_ref, weight_ref, residual_ref, mid_ref, squares_ref):
    projected = dot(weight_ref[...], heads_ref[...])
    mid = (residual_ref[...].astype(F32) + projected).astype(BF)
    mid_ref[...] = mid
    wide = mid.astype(F32)
    squares_ref[...] = jnp.broadcast_to(
        jnp.sum(wide * wide, axis=0, keepdims=True)[None], squares_ref.shape
    )


def hot_slots(targets_ref, k, first, rows):
    tokens = targets_ref.shape[1]
    slot_at = lax.broadcasted_iota(jnp.int32, (rows, tokens), 0) + first
    return targets_ref[k : k + 1] == slot_at


def normed_kernel(width, mid_ref, squares_ref, gain_ref, targets_ref, rows_ref, normed_ref):
    total = jnp.sum(squares_ref[...], axis=0)
    inverse = lax.rsqrt(total / width + EPSILON)
    normed = (mid_ref[...].astype(F32) * inverse * gain_ref[...]).astype(BF)
    normed_ref[...] = normed.astype(F32).T.astype(BF)
    chunk = rows_ref.shape[0] // 4
    for part in range(4):
        hot = hot_slots(targets_ref, 0, part * chunk, chunk) | hot_slots(
            targets_ref, 1, part * chunk, chunk
        )
        rows_ref[part * chunk : (part + 1) * chunk] = dot(
            hot.astype(F32).astype(BF), normed, NT
        ).astype(BF)


def sorting():
    to = lax.broadcasted_iota(jnp.int32, (320, 320), 0)
    frm = lax.broadcasted_iota(jnp.int32, (320, 320), 1)
    el = (to >= 80).astype(jnp.int32) + (to >= 160).astype(jnp.int32) + (to >= 240).astype(jnp.int32)
    within = to - el * 80
    src = jnp.zeros_like(to)
    for s in range(1, 8):
        src = src + (within >= s * 10).astype(jnp.int32)
    return (frm == src * 40 + el * 10 + within - src * 10).astype(F32).astype(BF)


def spread_kernel(arrived_ref, normed_ref, out_ref):
    order = sorting()
    for group in range(4):
        rows = dot(order, arrived_ref[group * 320 : (group + 1) * 320]).astype(BF)
        for el in range(4):
            piece = rows[el * 80 : (el + 1) * 80]
            for y in range(4):
                out_ref[y * 4 + el, group * 80 : (group + 1) * 80] = piece
    for x in range(4):
        piece = normed_ref[x * 128 : (x + 1) * 128]
        for y in range(4):
            out_ref[y * 4 + x, 320:448] = piece


def hidden_kernel(rows_ref, weight_ref, out_ref):
    expert = jnp.zeros((320, 256), F32)
    shared = jnp.zeros((128, 256), F32)

    def weights(first, cols):
        return jnp.concatenate(
            [weight_ref[x, g : g + 32, cols] for g in (first, first + 32) for x in range(4)], axis=0
        )

    for t in range(0, 16, 2):
        cols = slice(t * 128, (t + 2) * 128)
        rows = jnp.concatenate([rows_ref[t], rows_ref[t + 1]], axis=1)
        expert = expert + dot(rows[0:320], weights(0, cols), NT)
        shared = shared + dot(rows[320:448], weights(64, cols), NT)
    for first, count, both in ((0, 320, expert), (320, 128, shared)):
        gate, up = both[:, 0:128], both[:, 128:256]
        hidden = (gate / (1.0 + jnp.exp(-gate)) * up).astype(BF)
        for t in range(16):
            out_ref[t, first : first + count] = hidden


def down_kernel(hidden_ref, weight_ref, shared_ref, out_ref, shared_out_ref):
    order = sorting()
    produced = []
    for x in range(4):
        rows = jnp.zeros((320, 128), F32)
        shared = jnp.zeros((128, 128), F32)
        for y in range(0, 4, 2):
            cols = slice(y * 128, (y + 2) * 128)
            both = jnp.concatenate([hidden_ref[y * 4 + x], hidden_ref[y * 4 + 4 + x]], axis=1)
            rows = rows + dot(both[0:320], weight_ref[x, cols])
            shared = shared + dot(both[320:448], shared_ref[cols])
        produced.append(rows.astype(BF))
        shared_out_ref[x * 128 : (x + 1) * 128] = shared
    for group in range(4):
        rows = jnp.concatenate([p[group * 80 : (group + 1) * 80] for p in produced], axis=0)
        out_ref[group * 320 : (group + 1) * 320] = dot(order, rows, TN).astype(BF)


def last_kernel(returned_ref, targets_ref, weight_ref, mid_ref, shared_ref, out_ref):
    tokens = targets_ref.shape[1]
    total = mid_ref[...].astype(F32)
    slots = returned_ref.shape[0]
    chunk = slots // 5
    picked = [jnp.zeros(mid_ref.shape, F32) for _ in range(2)]
    for part in range(5):
        rows = returned_ref[part * chunk : (part + 1) * chunk]
        for k in range(2):
            hot = hot_slots(targets_ref, k, part * chunk, chunk).astype(F32).astype(BF)
            picked[k] = picked[k] + dot(rows, hot, TN)
    for k in range(2):
        total = total + picked[k] * weight_ref[k : k + 1]
    out_ref[...] = (total.T + shared_ref[...]).astype(BF)


def pieces(value):
    parts = []
    for _ in range(3):
        part = lax.reduce_precision(value, 8, 7)
        parts.append(part)
        value = value - part
    return jnp.concatenate(parts, axis=0).astype(BF)


def exchange(array, axis):
    return lax.all_to_all(array, axis, split_axis=0, concat_axis=0, tiled=True)


def shards(
    queries,
    key_vectors,
    value_vectors,
    log_gate_sums,
    residual,
    out_weight,
    norm_gain,
    routes,
    route_weight,
    expert_gate,
    expert_up,
    expert_down,
    shared_gate,
    shared_up,
    shared_down,
):
    tokens = queries.shape[0]
    width = norm_gain.shape[0]
    z, c = lax.axis_index("z"), lax.axis_index("c")
    tp = ("y", "x")
    gates = log_gate_sums.T
    ones = jnp.ones((3, tokens), BF)
    zeros = jnp.zeros((2, tokens), BF)
    block = jnp.concatenate(
        [key_vectors.T, pieces(-gates), ones, zeros, value_vectors.T], axis=0
    )
    query = jnp.concatenate([queries.T * BF(HDIM**-0.5), ones, pieces(gates), zeros], axis=0)
    query = jnp.concatenate([query, lax.ppermute(query, "c", ((0, 1), (1, 0)))], axis=1)
    state = (shape((1, 2 * tokens), F32), shape((72, 2 * tokens), F32))
    chips = lax.axis_size("z")
    ahead = [(i, i + 1) for i in range(chips - 1)]
    back = [(i, (i - 1) % chips) for i in range(chips)]

    local = jnp.stack([expert_gate, expert_up], axis=1).transpose(0, 1, 3, 2).reshape(4, 64, width)
    both = jnp.concatenate([shared_gate.T, shared_up.T], axis=0)
    local = jnp.concatenate([local, jnp.broadcast_to(both[None], (4, 64, width))], axis=1)
    up_weight = exchange(local, "x")
    targets = call(slots_kernel, shape((2, tokens), jnp.int32), routes.T)
    at = (lax.axis_index("y") * 4 + lax.axis_index("x")) * 128
    out_rows, residual = out_weight.T, residual.T
    gain = lax.dynamic_slice_in_dim(norm_gain, at, 128, 0).astype(F32)[:, None]

    prepared = (up_weight, targets, out_rows, residual, gain)

    up = down = block
    top, acc = call(own_kernel, state, c.reshape(1), block, query, smem=1)
    before = now = (top, acc)
    chip = z.reshape(1)
    for k in range(1, chips // 2 + 1):
        if k == 4:
            up, down, before, prepared = lax.optimization_barrier((up, down, before, prepared))
        elif k > 1:
            up, down, before = lax.optimization_barrier((up, down, before))
        up = lax.ppermute(up, "z", ahead)
        arrived, outs = [up], state
        if k < chips // 2:
            down = lax.ppermute(down, "z", back)
            arrived.append(down)
        else:
            outs = (*state, shape((80, tokens), F32))
        kernel = functools.partial(past_kernel, k, chips, len(arrived))
        before = now
        now = call(kernel, outs, chip, *arrived, query, *now, smem=1, flops=2**30)
    top, acc, sent = now
    up_weight, targets, out_rows, residual, gain = prepared
    other = lax.ppermute(sent, "c", ((0, 1), (1, 0)))
    heads = call(merge_kernel, shape((16, HDIM, tokens)), top, acc, other)
    heads = exchange(heads, tp)

    mid, squares = call(
        mid_kernel,
        (shape((128, tokens)), shape((16, 1, tokens), F32)),
        heads.reshape(16 * HDIM, tokens),
        out_rows,
        residual,
    )
    squares = exchange(squares, tp)
    rows, normed = call(
        lambda *refs: normed_kernel(width, *refs),
        (shape((1280, 128)), shape((tokens, 128))),
        mid,
        squares,
        gain,
        targets,
    )
    arrived = exchange(rows.reshape(32, 40, 128), ("z", "c")).reshape(1280, 128)
    spread = exchange(call(spread_kernel, shape((16, 448, 128)), arrived, normed), tp)
    hidden = exchange(call(hidden_kernel, shape((16, 448, 128)), spread, up_weight), tp)
    produced, shared = call(
        down_kernel,
        (shape((1280, 128)), shape((tokens, 128), F32)),
        hidden,
        expert_down,
        shared_down,
    )
    returned = exchange(produced.reshape(32, 40, 128), ("z", "c")).reshape(1280, 128)
    return call(
        last_kernel, shape((tokens, 128)), returned, targets, route_weight.T, mid, shared
    )


def solution(mesh):
    grid = Mesh(mesh.devices.reshape(16, 2, 4, 4), ("z", "c", "y", "x"))
    sp, tp = ("z", "c"), ("y", "x")
    placed = (
        P(sp, tp),
        P(sp, tp),
        P(sp, tp),
        P(sp, tp),
        P(sp, tp),
        P(None, tp),
        P(),
        P(sp, None),
        P(sp, None),
        P(sp, None, tp),
        P(sp, None, tp),
        P(sp, None, tp),
        P(None, tp),
        P(None, tp),
        P(None, tp),
    )
    return jax.shard_map(
        shards, mesh=grid, in_specs=placed, out_specs=P(sp, tp), check_vma=False
    )
```

```python
import functools

import jax
import jax.numpy as jnp
from jax import lax
from jax.experimental import pallas as pl
from jax.experimental.pallas import tpu as pltpu
from jax.sharding import Mesh, PartitionSpec as P


HDIM = 64
EPSILON = 1e-06
CAPACITY = 10
BF = jnp.bfloat16
F32 = jnp.float32
NN = (((1,), (0,)), ((), ()))
NT = (((1,), (1,)), ((), ()))
TN = (((0,), (0,)), ((), ()))


def dot(a, b, dims=NN):
    return lax.dot_general(a, b, dims, preferred_element_type=F32)


def call(kernel, outs, *args, smem=0, scratch=(), flops=2**28, nbytes=2**22, limit=2**24):
    specs = [pl.BlockSpec(memory_space=pltpu.SMEM)] * smem
    specs += [pl.BlockSpec(memory_space=pltpu.VMEM)] * (len(args) - smem)
    return pl.pallas_call(
        kernel,
        out_shape=outs,
        in_specs=specs,
        out_specs=jax.tree.map(lambda _: pl.BlockSpec(memory_space=pltpu.VMEM), outs),
        scratch_shapes=scratch,
        compiler_params=pltpu.CompilerParams(vmem_limit_bytes=limit),
        cost_estimate=pl.CostEstimate(flops=flops, bytes_accessed=nbytes, transcendentals=0),
    )(*args)


def shape(dims, dtype=BF):
    return jax.ShapeDtypeStruct(dims, dtype)


def fold(block, query_ref, top_ref, acc_ref, parts):
    half = query_ref.shape[1] // 4
    columns = [slice(part * half, (part + 1) * half) for part in parts]
    keys = block[0:72].astype(F32).T.astype(BF)
    scores = [dot(keys, query_ref[:, cols]) for cols in columns]
    old = [top_ref[:, cols] for cols in columns]
    new = [jnp.maximum(o, jnp.max(s, axis=0, keepdims=True)) for o, s in zip(old, scores)]
    weights = [jnp.exp(s - n).astype(BF) for s, n in zip(scores, new)]
    values = [
        acc_ref[:, cols] * jnp.exp(o - n) + dot(block[64:136], w)
        for cols, o, n, w in zip(columns, old, new, weights)
    ]
    for cols, n, v in zip(columns, new, values):
        top_ref[:, cols] = n
        acc_ref[:, cols] = v


def own_kernel(core_ref, block_ref, query_ref, top_ref, acc_ref):
    tokens = block_ref.shape[1]
    half = tokens // 2
    for part in range(2):
        cols = slice(part * half, (part + 1) * half)
        keys = (part + 1) * half
        key_at = lax.broadcasted_iota(jnp.int32, (keys, half), 0)
        query_at = lax.broadcasted_iota(jnp.int32, (keys, half), 1) + part * half
        scores = dot(block_ref[0:72, 0:keys], query_ref[:, cols], TN)
        scores = jnp.where(key_at <= query_at, scores, -1e30)
        top = jnp.max(scores, axis=0, keepdims=True)
        top_ref[:, cols] = top
        acc_ref[:, cols] = dot(block_ref[64:136, 0:keys], jnp.exp(scores - top).astype(BF))
    top_ref[:, tokens:] = jnp.full((1, tokens), -1e30, F32)
    acc_ref[:, tokens:] = jnp.zeros((72, tokens), F32)

    @pl.when(core_ref[0] == 0)
    def _():
        fold(block_ref[...], query_ref, top_ref, acc_ref, (2, 3))


def past_kernel(k, chips, count, chip_ref, *refs):
    blocks, query_ref = refs[0:count], refs[count]
    top_in, acc_in, top_ref, acc_ref = refs[1 + count : 5 + count]
    top_ref[...] = top_in[...]
    acc_ref[...] = acc_in[...]
    chip = chip_ref[0]
    for useful, block_ref in zip((chip + k >= chips, chip >= k)[-count:], blocks):

        @pl.when(useful)
        def _():
            fold(block_ref[...], query_ref, top_ref, acc_ref, range(4))

    if count == 1:
        sent_ref = refs[5 + count]
        tokens = sent_ref.shape[1]
        sent_ref[0:72] = acc_ref[:, tokens:]
        sent_ref[72:80] = jnp.broadcast_to(top_ref[:, tokens:], (8, tokens))


def merge_kernel(top_ref, acc_ref, other_ref, out_ref):
    tokens = out_ref.shape[2]
    top, other = top_ref[:, 0:tokens], other_ref[72:73]
    both = jnp.maximum(top, other)
    acc = acc_ref[:, 0:tokens] * jnp.exp(top - both) + other_ref[0:72] * jnp.exp(other - both)
    attended = (acc[8:72] / acc[3:4]).astype(BF)
    for t in range(16):
        out_ref[t] = attended


def slots_kernel(routes_ref, targets_ref):
    experts, tokens = 128, routes_ref.shape[1]
    expert_at = lax.broadcasted_iota(jnp.int32, (experts, tokens), 0)
    earlier = (
        lax.broadcasted_iota(jnp.int32, (tokens, tokens), 0)
        < lax.broadcasted_iota(jnp.int32, (tokens, tokens), 1)
    ).astype(F32).astype(BF)
    used = jnp.zeros((experts, 1), F32)
    for k in range(2):
        named = routes_ref[k : k + 1] == expert_at
        hot = named.astype(F32)
        before = dot(hot.astype(BF), earlier) + used
        rank = jnp.sum(jnp.where(named, before, 0.0), axis=0, keepdims=True)
        targets_ref[k : k + 1] = routes_ref[k : k + 1] * CAPACITY + rank.astype(jnp.int32)
        used = used + jnp.sum(hot, axis=1, keepdims=True)


def mid_kernel(heads_ref, weight_ref, residual_ref, mid_ref, squares_ref):
    projected = dot(weight_ref[...], heads_ref[...])
    mid = (residual_ref[...].astype(F32) + projected).astype(BF)
    mid_ref[...] = mid
    wide = mid.astype(F32)
    squares_ref[...] = jnp.broadcast_to(
        jnp.sum(wide * wide, axis=0, keepdims=True)[None], squares_ref.shape
    )


def hot_slots(targets_ref, k, first, rows):
    tokens = targets_ref.shape[1]
    slot_at = lax.broadcasted_iota(jnp.int32, (rows, tokens), 0) + first
    return targets_ref[k : k + 1] == slot_at


def normed_kernel(width, mid_ref, squares_ref, gain_ref, targets_ref, rows_ref, normed_ref):
    total = jnp.sum(squares_ref[...], axis=0)
    inverse = lax.rsqrt(total / width + EPSILON)
    normed = (mid_ref[...].astype(F32) * inverse * gain_ref[...]).astype(BF)
    normed_ref[...] = normed.astype(F32).T.astype(BF)
    chunk = rows_ref.shape[0] // 4
    for part in range(4):
        hot = hot_slots(targets_ref, 0, part * chunk, chunk) | hot_slots(
            targets_ref, 1, part * chunk, chunk
        )
        rows_ref[part * chunk : (part + 1) * chunk] = dot(
            hot.astype(F32).astype(BF), normed, NT
        ).astype(BF)


def sorting():
    to = lax.broadcasted_iota(jnp.int32, (320, 320), 0)
    frm = lax.broadcasted_iota(jnp.int32, (320, 320), 1)
    el = (to >= 80).astype(jnp.int32) + (to >= 160).astype(jnp.int32) + (to >= 240).astype(jnp.int32)
    within = to - el * 80
    src = jnp.zeros_like(to)
    for s in range(1, 8):
        src = src + (within >= s * 10).astype(jnp.int32)
    return (frm == src * 40 + el * 10 + within - src * 10).astype(F32).astype(BF)


def spread_kernel(arrived_ref, normed_ref, out_ref):
    order = sorting()
    for group in range(4):
        rows = dot(order, arrived_ref[group * 320 : (group + 1) * 320]).astype(BF)
        for el in range(4):
            piece = rows[el * 80 : (el + 1) * 80]
            for y in range(4):
                out_ref[y * 4 + el, group * 80 : (group + 1) * 80] = piece
    for x in range(4):
        piece = normed_ref[x * 128 : (x + 1) * 128]
        for y in range(4):
            out_ref[y * 4 + x, 320:448] = piece


def hidden_kernel(rows_ref, weight_ref, out_ref):
    expert = jnp.zeros((320, 256), F32)
    shared = jnp.zeros((128, 256), F32)

    def weights(first, cols):
        return jnp.concatenate(
            [weight_ref[x, g : g + 32, cols] for g in (first, first + 32) for x in range(4)], axis=0
        )

    for t in range(0, 16, 2):
        cols = slice(t * 128, (t + 2) * 128)
        rows = jnp.concatenate([rows_ref[t], rows_ref[t + 1]], axis=1)
        expert = expert + dot(rows[0:320], weights(0, cols), NT)
        shared = shared + dot(rows[320:448], weights(64, cols), NT)
    for first, count, both in ((0, 320, expert), (320, 128, shared)):
        gate, up = both[:, 0:128], both[:, 128:256]
        hidden = (gate / (1.0 + jnp.exp(-gate)) * up).astype(BF)
        for t in range(16):
            out_ref[t, first : first + count] = hidden


def down_kernel(hidden_ref, weight_ref, shared_ref, out_ref, shared_out_ref):
    order = sorting()
    produced = []
    for x in range(4):
        rows = jnp.zeros((320, 128), F32)
        shared = jnp.zeros((128, 128), F32)
        for y in range(0, 4, 2):
            cols = slice(y * 128, (y + 2) * 128)
            both = jnp.concatenate([hidden_ref[y * 4 + x], hidden_ref[y * 4 + 4 + x]], axis=1)
            rows = rows + dot(both[0:320], weight_ref[x, cols])
            shared = shared + dot(both[320:448], shared_ref[cols])
        produced.append(rows.astype(BF))
        shared_out_ref[x * 128 : (x + 1) * 128] = shared
    for group in range(4):
        rows = jnp.concatenate([p[group * 80 : (group + 1) * 80] for p in produced], axis=0)
        out_ref[group * 320 : (group + 1) * 320] = dot(order, rows, TN).astype(BF)


def last_kernel(returned_ref, targets_ref, weight_ref, mid_ref, shared_ref, out_ref):
    total = mid_ref[...].astype(F32)
    slots = returned_ref.shape[0]
    chunk = slots // 5
    picked = [jnp.zeros(mid_ref.shape, F32) for _ in range(2)]
    for part in range(5):
        rows = returned_ref[part * chunk : (part + 1) * chunk]
        for k in range(2):
            hot = hot_slots(targets_ref, k, part * chunk, chunk).astype(F32).astype(BF)
            picked[k] = picked[k] + dot(rows, hot, TN)
    for k in range(2):
        total = total + picked[k] * weight_ref[k : k + 1]
    out_ref[...] = (total.T + shared_ref[...]).astype(BF)


def pieces(value):
    parts = []
    for _ in range(3):
        part = lax.reduce_precision(value, 8, 7)
        parts.append(part)
        value = value - part
    return jnp.concatenate(parts, axis=0).astype(BF)


def exchange(array, axis):
    return lax.all_to_all(array, axis, split_axis=0, concat_axis=0, tiled=True)


def shards(
    queries,
    key_vectors,
    value_vectors,
    log_gate_sums,
    residual,
    out_weight,
    norm_gain,
    routes,
    route_weight,
    expert_gate,
    expert_up,
    expert_down,
    shared_gate,
    shared_up,
    shared_down,
):
    tokens = queries.shape[0]
    width = norm_gain.shape[0]
    z, c = lax.axis_index("z"), lax.axis_index("c")
    tp = ("y", "x")
    gates = log_gate_sums.T
    ones = jnp.ones((3, tokens), BF)
    zeros = jnp.zeros((2, tokens), BF)
    block = jnp.concatenate(
        [key_vectors.T, pieces(-gates), ones, zeros, value_vectors.T], axis=0
    )
    query = jnp.concatenate([queries.T * BF(HDIM**-0.5), ones, pieces(gates), zeros], axis=0)
    query = jnp.concatenate([query, lax.ppermute(query, "c", ((0, 1), (1, 0)))], axis=1)
    state = (shape((1, 2 * tokens), F32), shape((72, 2 * tokens), F32))
    chips = lax.axis_size("z")

    local = jnp.stack([expert_gate, expert_up], axis=1).transpose(0, 1, 3, 2).reshape(4, 64, width)
    both = jnp.concatenate([shared_gate.T, shared_up.T], axis=0)
    local = jnp.concatenate([local, jnp.broadcast_to(both[None], (4, 64, width))], axis=1)
    up_weight = exchange(local, "x")
    targets = call(slots_kernel, shape((2, tokens), jnp.int32), routes.T)
    at = (lax.axis_index("y") * 4 + lax.axis_index("x")) * 128
    out_rows, residual = out_weight.T, residual.T
    gain = lax.dynamic_slice_in_dim(norm_gain, at, 128, 0).astype(F32)[:, None]

    prepared = (up_weight, targets, out_rows, residual, gain)

    up = down = block
    top, acc = call(own_kernel, state, c.reshape(1), block, query, smem=1)
    before = now = (top, acc)
    chip = z.reshape(1)
    for k in range(1, chips // 2 + 1):
        if k == 4:
            up, down, before, prepared = lax.optimization_barrier((up, down, before, prepared))
        elif k > 1:
            up, down, before = lax.optimization_barrier((up, down, before))
        arrived, outs = [], state
        if k < chips // 2:
            back = [((i - k + 1) % chips, (i - k) % chips) for i in range(chips // 2 - 1)]
            down = lax.ppermute(down, "z", back)
            arrived.append(down)
        else:
            outs = (*state, shape((80, tokens), F32))
        up = lax.ppermute(up, "z", [(i, i + 1) for i in range(k - 1, chips - 1)])
        arrived.append(up)
        kernel = functools.partial(past_kernel, k, chips, len(arrived))
        before = now
        now = call(kernel, outs, chip, *arrived, query, *now, smem=1, flops=2**30)
    top, acc, sent = now
    up_weight, targets, out_rows, residual, gain = prepared
    other = lax.ppermute(sent, "c", ((0, 1), (1, 0)))
    heads = call(merge_kernel, shape((16, HDIM, tokens)), top, acc, other)
    heads = exchange(heads, tp)

    mid, squares = call(
        mid_kernel,
        (shape((128, tokens)), shape((16, 1, tokens), F32)),
        heads.reshape(16 * HDIM, tokens),
        out_rows,
        residual,
    )
    squares = exchange(squares, tp)
    rows, normed = call(
        lambda *refs: normed_kernel(width, *refs),
        (shape((1280, 128)), shape((tokens, 128))),
        mid,
        squares,
        gain,
        targets,
    )
    arrived = exchange(rows.reshape(32, 40, 128), ("z", "c")).reshape(1280, 128)
    spread = exchange(call(spread_kernel, shape((16, 448, 128)), arrived, normed), tp)
    hidden = exchange(call(hidden_kernel, shape((16, 448, 128)), spread, up_weight), tp)
    produced, shared = call(
        down_kernel,
        (shape((1280, 128)), shape((tokens, 128), F32)),
        hidden,
        expert_down,
        shared_down,
    )
    returned = exchange(produced.reshape(32, 40, 128), ("z", "c")).reshape(1280, 128)
    return call(
        last_kernel, shape((tokens, 128)), returned, targets, route_weight.T, mid, shared
    )


def solution(mesh):
    grid = Mesh(mesh.devices.reshape(16, 2, 4, 4), ("z", "c", "y", "x"))
    sp, tp = ("z", "c"), ("y", "x")
    placed = (
        P(sp, tp),
        P(sp, tp),
        P(sp, tp),
        P(sp, tp),
        P(sp, tp),
        P(None, tp),
        P(),
        P(sp, None),
        P(sp, None),
        P(sp, None, tp),
        P(sp, None, tp),
        P(sp, None, tp),
        P(None, tp),
        P(None, tp),
        P(None, tp),
    )
    return jax.shard_map(
        shards, mesh=grid, in_specs=placed, out_specs=P(sp, tp), check_vma=False
    )
```

```python
import functools

import jax
import jax.numpy as jnp
from jax import lax
from jax.experimental import pallas as pl
from jax.experimental.pallas import tpu as pltpu
from jax.sharding import Mesh, PartitionSpec as P


HDIM = 64
EPSILON = 1e-06
CAPACITY = 10
BF = jnp.bfloat16
F32 = jnp.float32
NN = (((1,), (0,)), ((), ()))
NT = (((1,), (1,)), ((), ()))
TN = (((0,), (0,)), ((), ()))


def dot(a, b, dims=NN):
    return lax.dot_general(a, b, dims, preferred_element_type=F32)


def call(kernel, outs, *args, smem=0, scratch=(), flops=2**28, nbytes=2**22, limit=2**24):
    specs = [pl.BlockSpec(memory_space=pltpu.SMEM)] * smem
    specs += [pl.BlockSpec(memory_space=pltpu.VMEM)] * (len(args) - smem)
    return pl.pallas_call(
        kernel,
        out_shape=outs,
        in_specs=specs,
        out_specs=jax.tree.map(lambda _: pl.BlockSpec(memory_space=pltpu.VMEM), outs),
        scratch_shapes=scratch,
        compiler_params=pltpu.CompilerParams(vmem_limit_bytes=limit),
        cost_estimate=pl.CostEstimate(flops=flops, bytes_accessed=nbytes, transcendentals=0),
    )(*args)


def shape(dims, dtype=BF):
    return jax.ShapeDtypeStruct(dims, dtype)


def fold(block, query_ref, top_ref, acc_ref, parts):
    half = query_ref.shape[1] // 4
    columns = [slice(part * half, (part + 1) * half) for part in parts]
    keys = block[0:72].astype(F32).T.astype(BF)
    scores = [dot(keys, query_ref[:, cols]) for cols in columns]
    old = [top_ref[:, cols] for cols in columns]
    new = [jnp.maximum(o, jnp.max(s, axis=0, keepdims=True)) for o, s in zip(old, scores)]
    weights = [jnp.exp(s - n).astype(BF) for s, n in zip(scores, new)]
    values = [
        acc_ref[:, cols] * jnp.exp(o - n) + dot(block[64:136], w)
        for cols, o, n, w in zip(columns, old, new, weights)
    ]
    for cols, n, v in zip(columns, new, values):
        top_ref[:, cols] = n
        acc_ref[:, cols] = v


def own_kernel(core_ref, block_ref, query_ref, top_ref, acc_ref):
    tokens = block_ref.shape[1]
    half = tokens // 2
    for part in range(2):
        cols = slice(part * half, (part + 1) * half)
        keys = (part + 1) * half
        key_at = lax.broadcasted_iota(jnp.int32, (keys, half), 0)
        query_at = lax.broadcasted_iota(jnp.int32, (keys, half), 1) + part * half
        scores = dot(block_ref[0:72, 0:keys], query_ref[:, cols], TN)
        scores = jnp.where(key_at <= query_at, scores, -1e30)
        top = jnp.max(scores, axis=0, keepdims=True)
        top_ref[:, cols] = top
        acc_ref[:, cols] = dot(block_ref[64:136, 0:keys], jnp.exp(scores - top).astype(BF))
    top_ref[:, tokens:] = jnp.full((1, tokens), -1e30, F32)
    acc_ref[:, tokens:] = jnp.zeros((72, tokens), F32)

    @pl.when(core_ref[0] == 0)
    def _():
        fold(block_ref[...], query_ref, top_ref, acc_ref, (2, 3))


def past_kernel(k, chips, count, chip_ref, *refs):
    blocks, query_ref = refs[0:count], refs[count]
    top_in, acc_in, top_ref, acc_ref = refs[1 + count : 5 + count]
    top_ref[...] = top_in[...]
    acc_ref[...] = acc_in[...]
    chip = chip_ref[0]
    for useful, block_ref in zip((chip + k >= chips, chip >= k)[-count:], blocks):

        @pl.when(useful)
        def _():
            fold(block_ref[...], query_ref, top_ref, acc_ref, range(4))

    if count == 1:
        sent_ref = refs[5 + count]
        tokens = sent_ref.shape[1]
        sent_ref[0:72] = acc_ref[:, tokens:]
        sent_ref[72:80] = jnp.broadcast_to(top_ref[:, tokens:], (8, tokens))


def merge_kernel(top_ref, acc_ref, other_ref, out_ref):
    tokens = out_ref.shape[2]
    top, other = top_ref[:, 0:tokens], other_ref[72:73]
    both = jnp.maximum(top, other)
    acc = acc_ref[:, 0:tokens] * jnp.exp(top - both) + other_ref[0:72] * jnp.exp(other - both)
    attended = (acc[8:72] / acc[3:4]).astype(BF)
    for t in range(16):
        out_ref[t] = attended


def slots_kernel(routes_ref, targets_ref):
    experts, tokens = 128, routes_ref.shape[1]
    expert_at = lax.broadcasted_iota(jnp.int32, (experts, tokens), 0)
    earlier = (
        lax.broadcasted_iota(jnp.int32, (tokens, tokens), 0)
        < lax.broadcasted_iota(jnp.int32, (tokens, tokens), 1)
    ).astype(F32).astype(BF)
    used = jnp.zeros((experts, 1), F32)
    for k in range(2):
        named = routes_ref[k : k + 1] == expert_at
        hot = named.astype(F32)
        before = dot(hot.astype(BF), earlier) + used
        rank = jnp.sum(jnp.where(named, before, 0.0), axis=0, keepdims=True)
        targets_ref[k : k + 1] = routes_ref[k : k + 1] * CAPACITY + rank.astype(jnp.int32)
        used = used + jnp.sum(hot, axis=1, keepdims=True)


def hot_slots(targets_ref, k, first, rows):
    tokens = targets_ref.shape[1]
    slot_at = lax.broadcasted_iota(jnp.int32, (rows, tokens), 0) + first
    return targets_ref[k : k + 1] == slot_at


def mid_kernel(heads_ref, weight_ref, residual_ref, targets_ref, mid_ref, rows_ref, own_ref):
    projected = dot(weight_ref[...], heads_ref[...])
    mid = (residual_ref[...].astype(F32) + projected).astype(BF)
    mid_ref[...] = mid
    own_ref[...] = mid.astype(F32).T.astype(BF)
    chunk = rows_ref.shape[0] // 4
    for part in range(4):
        hot = hot_slots(targets_ref, 0, part * chunk, chunk) | hot_slots(
            targets_ref, 1, part * chunk, chunk
        )
        rows_ref[part * chunk : (part + 1) * chunk] = dot(
            hot.astype(F32).astype(BF), mid, NT
        ).astype(BF)


def sorting():
    to = lax.broadcasted_iota(jnp.int32, (320, 320), 0)
    frm = lax.broadcasted_iota(jnp.int32, (320, 320), 1)
    el = (to >= 80).astype(jnp.int32) + (to >= 160).astype(jnp.int32) + (to >= 240).astype(jnp.int32)
    within = to - el * 80
    src = jnp.zeros_like(to)
    for s in range(1, 8):
        src = src + (within >= s * 10).astype(jnp.int32)
    return (frm == src * 40 + el * 10 + within - src * 10).astype(F32).astype(BF)


def spread_kernel(arrived_ref, own_ref, out_ref):
    order = sorting()
    for group in range(4):
        rows = dot(order, arrived_ref[group * 320 : (group + 1) * 320]).astype(BF)
        for el in range(4):
            piece = rows[el * 80 : (el + 1) * 80]
            for y in range(4):
                out_ref[y * 4 + el, group * 80 : (group + 1) * 80] = piece
    for x in range(4):
        piece = own_ref[x * 128 : (x + 1) * 128]
        for y in range(4):
            out_ref[y * 4 + x, 320:448] = piece


def hidden_kernel(rows_ref, weight_ref, gain_ref, out_ref):
    squares = jnp.zeros(rows_ref.shape[1:], F32)
    for t in range(16):
        wide = rows_ref[t].astype(F32)
        squares = squares + wide * wide
    total = jnp.sum(squares, axis=1, keepdims=True)
    inverse = lax.rsqrt(total / gain_ref.shape[1] + EPSILON)

    def normed(t):
        gain = gain_ref[:, t * 128 : (t + 1) * 128].astype(F32)
        return (rows_ref[t].astype(F32) * inverse * gain).astype(BF)

    expert = jnp.zeros((320, 256), F32)
    shared = jnp.zeros((128, 256), F32)

    def weights(first, cols):
        return jnp.concatenate(
            [weight_ref[x, g : g + 32, cols] for g in (first, first + 32) for x in range(4)], axis=0
        )

    for t in range(0, 16, 2):
        cols = slice(t * 128, (t + 2) * 128)
        rows = jnp.concatenate([normed(t), normed(t + 1)], axis=1)
        expert = expert + dot(rows[0:320], weights(0, cols), NT)
        shared = shared + dot(rows[320:448], weights(64, cols), NT)
    for first, count, both in ((0, 320, expert), (320, 128, shared)):
        gate, up = both[:, 0:128], both[:, 128:256]
        hidden = (gate / (1.0 + jnp.exp(-gate)) * up).astype(BF)
        for t in range(16):
            out_ref[t, first : first + count] = hidden


def down_kernel(hidden_ref, weight_ref, shared_ref, out_ref, shared_out_ref):
    order = sorting()
    produced = []
    for x in range(4):
        rows = jnp.zeros((320, 128), F32)
        shared = jnp.zeros((128, 128), F32)
        for y in range(0, 4, 2):
            cols = slice(y * 128, (y + 2) * 128)
            both = jnp.concatenate([hidden_ref[y * 4 + x], hidden_ref[y * 4 + 4 + x]], axis=1)
            rows = rows + dot(both[0:320], weight_ref[x, cols])
            shared = shared + dot(both[320:448], shared_ref[cols])
        produced.append(rows.astype(BF))
        shared_out_ref[x * 128 : (x + 1) * 128] = shared
    for group in range(4):
        rows = jnp.concatenate([p[group * 80 : (group + 1) * 80] for p in produced], axis=0)
        out_ref[group * 320 : (group + 1) * 320] = dot(order, rows, TN).astype(BF)


def last_kernel(returned_ref, targets_ref, weight_ref, mid_ref, shared_ref, out_ref):
    total = mid_ref[...].astype(F32)
    slots = returned_ref.shape[0]
    chunk = slots // 5
    picked = [jnp.zeros(mid_ref.shape, F32) for _ in range(2)]
    for part in range(5):
        rows = returned_ref[part * chunk : (part + 1) * chunk]
        for k in range(2):
            hot = hot_slots(targets_ref, k, part * chunk, chunk).astype(F32).astype(BF)
            picked[k] = picked[k] + dot(rows, hot, TN)
    for k in range(2):
        total = total + picked[k] * weight_ref[k : k + 1]
    out_ref[...] = (total.T + shared_ref[...]).astype(BF)


def pieces(value):
    parts = []
    for _ in range(3):
        part = lax.reduce_precision(value, 8, 7)
        parts.append(part)
        value = value - part
    return jnp.concatenate(parts, axis=0).astype(BF)


def exchange(array, axis):
    return lax.all_to_all(array, axis, split_axis=0, concat_axis=0, tiled=True)


def shards(
    queries,
    key_vectors,
    value_vectors,
    log_gate_sums,
    residual,
    out_weight,
    norm_gain,
    routes,
    route_weight,
    expert_gate,
    expert_up,
    expert_down,
    shared_gate,
    shared_up,
    shared_down,
):
    tokens = queries.shape[0]
    width = norm_gain.shape[0]
    z, c = lax.axis_index("z"), lax.axis_index("c")
    tp = ("y", "x")
    gates = log_gate_sums.T
    ones = jnp.ones((3, tokens), BF)
    zeros = jnp.zeros((2, tokens), BF)
    block = jnp.concatenate(
        [key_vectors.T, pieces(-gates), ones, zeros, value_vectors.T], axis=0
    )
    query = jnp.concatenate([queries.T * BF(HDIM**-0.5), ones, pieces(gates), zeros], axis=0)
    query = jnp.concatenate([query, lax.ppermute(query, "c", ((0, 1), (1, 0)))], axis=1)
    state = (shape((1, 2 * tokens), F32), shape((72, 2 * tokens), F32))
    chips = lax.axis_size("z")

    local = jnp.stack([expert_gate, expert_up], axis=1).transpose(0, 1, 3, 2).reshape(4, 64, width)
    both = jnp.concatenate([shared_gate.T, shared_up.T], axis=0)
    local = jnp.concatenate([local, jnp.broadcast_to(both[None], (4, 64, width))], axis=1)
    targets = call(slots_kernel, shape((2, tokens), jnp.int32), routes.T)
    out_rows, residual = out_weight.T, residual.T
    gain = norm_gain.astype(F32)[None]
    prepared = (targets, out_rows, residual, gain)

    up = down = block
    top, acc = call(own_kernel, state, c.reshape(1), block, query, smem=1)
    before = now = (top, acc)
    chip = z.reshape(1)
    for k in range(1, chips // 2 + 1):
        if k == 2:
            up, down, before, local = lax.optimization_barrier((up, down, before, local))
        elif k == 5:
            up, down, before, prepared = lax.optimization_barrier((up, down, before, prepared))
        elif k == 6:
            up, down, before, up_weight = lax.optimization_barrier((up, down, before, up_weight))
        elif k > 1:
            up, down, before = lax.optimization_barrier((up, down, before))
        arrived, outs = [], state
        if k < chips // 2:
            back = [((i - k + 1) % chips, (i - k) % chips) for i in range(chips // 2 - 1)]
            down = lax.ppermute(down, "z", back)
            arrived.append(down)
        else:
            outs = (*state, shape((80, tokens), F32))
        up = lax.ppermute(up, "z", [(i, i + 1) for i in range(k - 1, chips - 1)])
        arrived.append(up)
        if k == 2:
            up_weight = exchange(local, "x")
        kernel = functools.partial(past_kernel, k, chips, len(arrived))
        before = now
        now = call(kernel, outs, chip, *arrived, query, *now, smem=1, flops=2**30)
    top, acc, sent = now
    targets, out_rows, residual, gain = prepared
    other = lax.ppermute(sent, "c", ((0, 1), (1, 0)))
    heads = call(merge_kernel, shape((16, HDIM, tokens)), top, acc, other)
    heads = exchange(heads, tp)

    mid, rows, own = call(
        mid_kernel,
        (shape((128, tokens)), shape((1280, 128)), shape((tokens, 128))),
        heads.reshape(16 * HDIM, tokens),
        out_rows,
        residual,
        targets,
    )
    arrived = exchange(rows.reshape(32, 40, 128), ("z", "c")).reshape(1280, 128)
    spread = exchange(call(spread_kernel, shape((16, 448, 128)), arrived, own), tp)
    hidden = exchange(call(hidden_kernel, shape((16, 448, 128)), spread, up_weight, gain), tp)
    produced, shared = call(
        down_kernel,
        (shape((1280, 128)), shape((tokens, 128), F32)),
        hidden,
        expert_down,
        shared_down,
    )
    returned = exchange(produced.reshape(32, 40, 128), ("z", "c")).reshape(1280, 128)
    return call(
        last_kernel, shape((tokens, 128)), returned, targets, route_weight.T, mid, shared
    )


def solution(mesh):
    grid = Mesh(mesh.devices.reshape(16, 2, 4, 4), ("z", "c", "y", "x"))
    sp, tp = ("z", "c"), ("y", "x")
    placed = (
        P(sp, tp),
        P(sp, tp),
        P(sp, tp),
        P(sp, tp),
        P(sp, tp),
        P(None, tp),
        P(),
        P(sp, None),
        P(sp, None),
        P(sp, None, tp),
        P(sp, None, tp),
        P(sp, None, tp),
        P(None, tp),
        P(None, tp),
        P(None, tp),
    )
    return jax.shard_map(
        shards, mesh=grid, in_specs=placed, out_specs=P(sp, tp), check_vma=False
    )
```

```python
import functools

import jax
import jax.numpy as jnp
from jax import lax
from jax.experimental import pallas as pl
from jax.experimental.pallas import tpu as pltpu
from jax.sharding import Mesh, PartitionSpec as P


HDIM = 64
EPSILON = 1e-06
CAPACITY = 10
BF = jnp.bfloat16
F32 = jnp.float32
NN = (((1,), (0,)), ((), ()))
NT = (((1,), (1,)), ((), ()))
TN = (((0,), (0,)), ((), ()))


def dot(a, b, dims=NN):
    return lax.dot_general(a, b, dims, preferred_element_type=F32)


def call(kernel, outs, *args, smem=0, scratch=(), flops=2**28, nbytes=2**22, limit=2**24):
    specs = [pl.BlockSpec(memory_space=pltpu.SMEM)] * smem
    specs += [pl.BlockSpec(memory_space=pltpu.VMEM)] * (len(args) - smem)
    return pl.pallas_call(
        kernel,
        out_shape=outs,
        in_specs=specs,
        out_specs=jax.tree.map(lambda _: pl.BlockSpec(memory_space=pltpu.VMEM), outs),
        scratch_shapes=scratch,
        compiler_params=pltpu.CompilerParams(vmem_limit_bytes=limit),
        cost_estimate=pl.CostEstimate(flops=flops, bytes_accessed=nbytes, transcendentals=0),
    )(*args)


def shape(dims, dtype=BF):
    return jax.ShapeDtypeStruct(dims, dtype)


def fold(block, query_ref, top_ref, acc_ref, parts):
    half = query_ref.shape[1] // 4
    columns = [slice(part * half, (part + 1) * half) for part in parts]
    keys = block[0:72].astype(F32).T.astype(BF)
    scores = [dot(keys, query_ref[:, cols]) for cols in columns]
    old = [top_ref[:, cols] for cols in columns]
    new = [jnp.maximum(o, jnp.max(s, axis=0, keepdims=True)) for o, s in zip(old, scores)]
    weights = [jnp.exp(s - n).astype(BF) for s, n in zip(scores, new)]
    values = [
        acc_ref[:, cols] * jnp.exp(o - n) + dot(block[64:136], w)
        for cols, o, n, w in zip(columns, old, new, weights)
    ]
    for cols, n, v in zip(columns, new, values):
        top_ref[:, cols] = n
        acc_ref[:, cols] = v


def own_kernel(core_ref, block_ref, query_ref, top_ref, acc_ref):
    tokens = block_ref.shape[1]
    half = tokens // 2
    for part in range(2):
        cols = slice(part * half, (part + 1) * half)
        keys = (part + 1) * half
        key_at = lax.broadcasted_iota(jnp.int32, (keys, half), 0)
        query_at = lax.broadcasted_iota(jnp.int32, (keys, half), 1) + part * half
        scores = dot(block_ref[0:72, 0:keys], query_ref[:, cols], TN)
        scores = jnp.where(key_at <= query_at, scores, -1e30)
        top = jnp.max(scores, axis=0, keepdims=True)
        top_ref[:, cols] = top
        acc_ref[:, cols] = dot(block_ref[64:136, 0:keys], jnp.exp(scores - top).astype(BF))
    top_ref[:, tokens:] = jnp.full((1, tokens), -1e30, F32)
    acc_ref[:, tokens:] = jnp.zeros((72, tokens), F32)

    @pl.when(core_ref[0] == 0)
    def _():
        fold(block_ref[...], query_ref, top_ref, acc_ref, (2, 3))


def past_kernel(k, chips, count, chip_ref, *refs):
    blocks, query_ref = refs[0:count], refs[count]
    top_in, acc_in, top_ref, acc_ref = refs[1 + count : 5 + count]
    top_ref[...] = top_in[...]
    acc_ref[...] = acc_in[...]
    chip = chip_ref[0]
    for useful, block_ref in zip((chip + k >= chips, chip >= k)[-count:], blocks):

        @pl.when(useful)
        def _():
            fold(block_ref[...], query_ref, top_ref, acc_ref, range(4))

    if count == 1:
        sent_ref = refs[5 + count]
        tokens = sent_ref.shape[1]
        sent_ref[0:72] = acc_ref[:, tokens:]
        sent_ref[72:80] = jnp.broadcast_to(top_ref[:, tokens:], (8, tokens))


def merge_kernel(top_ref, acc_ref, other_ref, out_ref):
    tokens = out_ref.shape[2]
    top, other = top_ref[:, 0:tokens], other_ref[72:73]
    both = jnp.maximum(top, other)
    acc = acc_ref[:, 0:tokens] * jnp.exp(top - both) + other_ref[0:72] * jnp.exp(other - both)
    attended = (acc[8:72] / acc[3:4]).astype(BF)
    for t in range(16):
        out_ref[t] = attended


def slots_kernel(routes_ref, targets_ref):
    experts, tokens = 128, routes_ref.shape[1]
    expert_at = lax.broadcasted_iota(jnp.int32, (experts, tokens), 0)
    earlier = (
        lax.broadcasted_iota(jnp.int32, (tokens, tokens), 0)
        < lax.broadcasted_iota(jnp.int32, (tokens, tokens), 1)
    ).astype(F32).astype(BF)
    used = jnp.zeros((experts, 1), F32)
    for k in range(2):
        named = routes_ref[k : k + 1] == expert_at
        hot = named.astype(F32)
        before = dot(hot.astype(BF), earlier) + used
        rank = jnp.sum(jnp.where(named, before, 0.0), axis=0, keepdims=True)
        targets_ref[k : k + 1] = routes_ref[k : k + 1] * CAPACITY + rank.astype(jnp.int32)
        used = used + jnp.sum(hot, axis=1, keepdims=True)


def hot_slots(targets_ref, k, first, rows):
    tokens = targets_ref.shape[1]
    slot_at = lax.broadcasted_iota(jnp.int32, (rows, tokens), 0) + first
    return targets_ref[k : k + 1] == slot_at


def mid_kernel(heads_ref, weight_ref, residual_ref, targets_ref, mid_ref, rows_ref, own_ref):
    projected = dot(weight_ref[...], heads_ref[...])
    mid = (residual_ref[...].astype(F32) + projected).astype(BF)
    mid_ref[...] = mid
    own_ref[...] = mid.astype(F32).T.astype(BF)
    chunk = rows_ref.shape[0] // 4
    for part in range(4):
        hot = hot_slots(targets_ref, 0, part * chunk, chunk) | hot_slots(
            targets_ref, 1, part * chunk, chunk
        )
        rows_ref[part * chunk : (part + 1) * chunk] = dot(
            hot.astype(F32).astype(BF), mid, NT
        ).astype(BF)


def sorting():
    to = lax.broadcasted_iota(jnp.int32, (320, 320), 0)
    frm = lax.broadcasted_iota(jnp.int32, (320, 320), 1)
    el = (to >= 80).astype(jnp.int32) + (to >= 160).astype(jnp.int32) + (to >= 240).astype(jnp.int32)
    within = to - el * 80
    src = jnp.zeros_like(to)
    for s in range(1, 8):
        src = src + (within >= s * 10).astype(jnp.int32)
    return (frm == src * 40 + el * 10 + within - src * 10).astype(F32).astype(BF)


def spread_kernel(arrived_ref, own_ref, out_ref):
    order = sorting()
    for group in range(4):
        rows = dot(order, arrived_ref[group * 320 : (group + 1) * 320]).astype(BF)
        for el in range(4):
            piece = rows[el * 80 : (el + 1) * 80]
            for y in range(4):
                out_ref[y * 4 + el, group * 80 : (group + 1) * 80] = piece
    for x in range(4):
        piece = own_ref[x * 128 : (x + 1) * 128]
        for y in range(4):
            out_ref[y * 4 + x, 320:448] = piece


def hidden_kernel(rows_ref, weight_ref, gain_ref, out_ref):
    squares = jnp.zeros(rows_ref.shape[1:], F32)
    for t in range(16):
        wide = rows_ref[t].astype(F32)
        squares = squares + wide * wide
    total = jnp.sum(squares, axis=1, keepdims=True)
    inverse = lax.rsqrt(total / gain_ref.shape[1] + EPSILON)

    def normed(t):
        gain = gain_ref[:, t * 128 : (t + 1) * 128].astype(F32)
        return (rows_ref[t].astype(F32) * inverse * gain).astype(BF)

    expert = jnp.zeros((320, 256), F32)
    shared = jnp.zeros((128, 256), F32)

    def weights(first, cols):
        return jnp.concatenate(
            [weight_ref[x, g : g + 32, cols] for g in (first, first + 32) for x in range(4)], axis=0
        )

    for t in range(0, 16, 2):
        cols = slice(t * 128, (t + 2) * 128)
        rows = jnp.concatenate([normed(t), normed(t + 1)], axis=1)
        expert = expert + dot(rows[0:320], weights(0, cols), NT)
        shared = shared + dot(rows[320:448], weights(64, cols), NT)
    for first, count, both in ((0, 320, expert), (320, 128, shared)):
        gate, up = both[:, 0:128], both[:, 128:256]
        hidden = (gate / (1.0 + jnp.exp(-gate)) * up).astype(BF)
        for t in range(16):
            out_ref[t, first : first + count] = hidden


def down_kernel(hidden_ref, weight_ref, shared_ref, out_ref, shared_out_ref):
    order = sorting()
    produced = []
    for x in range(4):
        rows = jnp.zeros((320, 128), F32)
        shared = jnp.zeros((128, 128), F32)
        for y in range(0, 4, 2):
            cols = slice(y * 128, (y + 2) * 128)
            both = jnp.concatenate([hidden_ref[y * 4 + x], hidden_ref[y * 4 + 4 + x]], axis=1)
            rows = rows + dot(both[0:320], weight_ref[x, cols])
            shared = shared + dot(both[320:448], shared_ref[cols])
        produced.append(rows.astype(BF))
        shared_out_ref[x * 128 : (x + 1) * 128] = shared
    for group in range(4):
        rows = jnp.concatenate([p[group * 80 : (group + 1) * 80] for p in produced], axis=0)
        out_ref[group * 320 : (group + 1) * 320] = dot(order, rows, TN).astype(BF)


def last_kernel(returned_ref, targets_ref, weight_ref, mid_ref, shared_ref, out_ref):
    total = mid_ref[...].astype(F32)
    slots = returned_ref.shape[0]
    chunk = slots // 5
    picked = [jnp.zeros(mid_ref.shape, F32) for _ in range(2)]
    for part in range(5):
        rows = returned_ref[part * chunk : (part + 1) * chunk]
        for k in range(2):
            hot = hot_slots(targets_ref, k, part * chunk, chunk).astype(F32).astype(BF)
            picked[k] = picked[k] + dot(rows, hot, TN)
    for k in range(2):
        total = total + picked[k] * weight_ref[k : k + 1]
    out_ref[...] = (total.T + shared_ref[...]).astype(BF)


def pieces(value):
    parts = []
    for _ in range(3):
        part = lax.reduce_precision(value, 8, 7)
        parts.append(part)
        value = value - part
    return jnp.concatenate(parts, axis=0).astype(BF)


def exchange(array, axis):
    return lax.all_to_all(array, axis, split_axis=0, concat_axis=0, tiled=True)


def shards(
    queries,
    key_vectors,
    value_vectors,
    log_gate_sums,
    residual,
    out_weight,
    norm_gain,
    routes,
    route_weight,
    expert_gate,
    expert_up,
    expert_down,
    shared_gate,
    shared_up,
    shared_down,
):
    tokens = queries.shape[0]
    width = norm_gain.shape[0]
    z, c = lax.axis_index("z"), lax.axis_index("c")
    tp = ("y", "x")
    gates = log_gate_sums.T
    ones = jnp.ones((3, tokens), BF)
    zeros = jnp.zeros((2, tokens), BF)
    block = jnp.concatenate(
        [key_vectors.T, pieces(-gates), ones, zeros, value_vectors.T], axis=0
    )
    query = jnp.concatenate([queries.T * BF(HDIM**-0.5), ones, pieces(gates), zeros], axis=0)
    query = jnp.concatenate([query, lax.ppermute(query, "c", ((0, 1), (1, 0)))], axis=1)
    state = (shape((1, 2 * tokens), F32), shape((72, 2 * tokens), F32))
    chips = lax.axis_size("z")

    local = jnp.stack([expert_gate, expert_up], axis=1).transpose(0, 1, 3, 2).reshape(4, 64, width)
    both = jnp.concatenate([shared_gate.T, shared_up.T], axis=0)
    local = jnp.concatenate([local, jnp.broadcast_to(both[None], (4, 64, width))], axis=1)
    targets = call(slots_kernel, shape((2, tokens), jnp.int32), routes.T)
    out_rows, residual = out_weight.T, residual.T
    gain = norm_gain.astype(F32)[None]
    prepared = (targets, out_rows, residual, gain)

    up = down = block
    top, acc = call(own_kernel, state, c.reshape(1), block, query, smem=1)
    before = now = (top, acc)
    chip = z.reshape(1)
    for k in range(1, chips // 2 + 1):
        if k == 2:
            down, before, local = lax.optimization_barrier((down, before, local))
        elif k == 5:
            down, before, prepared = lax.optimization_barrier((down, before, prepared))
        elif k == 6:
            down, before, up_weight = lax.optimization_barrier((down, before, up_weight))
        elif 1 < k < chips // 2:
            down, before = lax.optimization_barrier((down, before))
        if k > 1:
            up, before = lax.optimization_barrier((up, before))
        arrived, outs = [], state
        if k < chips // 2:
            back = [((i - k + 1) % chips, (i - k) % chips) for i in range(chips // 2 - 1)]
            down = lax.ppermute(down, "z", back)
            arrived.append(down)
        else:
            outs = (*state, shape((80, tokens), F32))
        up = lax.ppermute(up, "z", [(i, i + 1) for i in range(k - 1, chips - 1)])
        arrived.append(up)
        if k == 2:
            up_weight = exchange(local, "x")
        kernel = functools.partial(past_kernel, k, chips, len(arrived))
        before = now
        now = call(kernel, outs, chip, *arrived, query, *now, smem=1, flops=2**30)
    top, acc, sent = now
    targets, out_rows, residual, gain = prepared
    other = lax.ppermute(sent, "c", ((0, 1), (1, 0)))
    heads = call(merge_kernel, shape((16, HDIM, tokens)), top, acc, other)
    heads = exchange(heads, tp)

    mid, rows, own = call(
        mid_kernel,
        (shape((128, tokens)), shape((1280, 128)), shape((tokens, 128))),
        heads.reshape(16 * HDIM, tokens),
        out_rows,
        residual,
        targets,
    )
    arrived = exchange(rows.reshape(32, 40, 128), ("z", "c")).reshape(1280, 128)
    spread = exchange(call(spread_kernel, shape((16, 448, 128)), arrived, own), tp)
    hidden = exchange(call(hidden_kernel, shape((16, 448, 128)), spread, up_weight, gain), tp)
    produced, shared = call(
        down_kernel,
        (shape((1280, 128)), shape((tokens, 128), F32)),
        hidden,
        expert_down,
        shared_down,
    )
    returned = exchange(produced.reshape(32, 40, 128), ("z", "c")).reshape(1280, 128)
    return call(
        last_kernel, shape((tokens, 128)), returned, targets, route_weight.T, mid, shared
    )


def solution(mesh):
    grid = Mesh(mesh.devices.reshape(16, 2, 4, 4), ("z", "c", "y", "x"))
    sp, tp = ("z", "c"), ("y", "x")
    placed = (
        P(sp, tp),
        P(sp, tp),
        P(sp, tp),
        P(sp, tp),
        P(sp, tp),
        P(None, tp),
        P(),
        P(sp, None),
        P(sp, None),
        P(sp, None, tp),
        P(sp, None, tp),
        P(sp, None, tp),
        P(None, tp),
        P(None, tp),
        P(None, tp),
    )
    return jax.shard_map(
        shards, mesh=grid, in_specs=placed, out_specs=P(sp, tp), check_vma=False
    )
```
